32 devices in a mesh: grp: 2 (over y), sp: 4 (over z), tp: 4 (over x, core).
Axes of the slice: x: 2, y: 2, z: 4, core: 2. Of those that a mesh axis runs over, the one named last changes fastest.
Arguments:
- stream: bfloat16 [3072, 4096], P(('grp', 'sp'), 'tp'), parts along dimension 0, may hold values from -6 to 6
- norm_gain: bfloat16 [2, 4096], replicated, may hold values from 0.099609375 to 1.8984375
- w_signal: bfloat16 [2, 4096, 1024], P(None, 'sp', 'tp'), may hold values from -0.09375 to 0.09375
- w_gate: bfloat16 [2, 4096, 1024], P(None, 'sp', 'tp'), may hold values from -0.09375 to 0.09375
- conv_taps: bfloat16 [2, 31, 1024], P(None, None, 'tp'), may hold values from -4 to 4
- conv_bias: bfloat16 [2, 1024], P(None, 'tp'), may hold values from -3 to 3
- ln_gain: bfloat16 [2, 1024], P(None, 'tp'), may hold values from 0.099609375 to 1.8984375
- ln_shift: bfloat16 [2, 1024], P(None, 'tp'), may hold values from -3 to 3
- w_out: bfloat16 [2, 1024, 4096], P(None, 'sp', 'tp'), may hold values from -0.375 to 0.375
Outputs:
- mixed_stream: bfloat16 [3072, 4096], P(('grp', 'sp'), 'tp'), parts along dimension 0
The draws below stay inside these ranges and needn't reach their ends.
There are 2 independent parts, one for each index of `grp`. The reference program is written for one: setup_inputs(seed, part) draws one part's arguments, and reference() takes and returns one part's arrays. A program takes and returns all parts, laid end to end along the dimension named above; an argument that names none is the same for every part. Nothing has to cross between parts.
All inputs are finite; a program needn't handle non-finite values.
Results may differ from the reference program's by a relative error of at most 0.01.
Values may be sent and summed in bfloat16 or wider, within the bound.
A program may use at most 64 MiB of HBM per device.

```python
import jax
import jax.numpy as jnp
from jax import lax

D = 4096
C = 1024
KERNEL = 31
LAYERS = 2
TOKENS = 1536


def draw_conv_taps(key, part):
    key_base = jax.random.fold_in(key, 11)
    key_scale = jax.random.fold_in(key, 12)
    base = jnp.clip(jax.random.normal(key_base, (LAYERS, KERNEL, C), jnp.float32), -4.0, 4.0) * KERNEL ** (-0.5)
    log_scale = jax.random.uniform(key_scale, (LAYERS, 8), jnp.float32, jnp.log(0.3), jnp.log(3.0))
    scales = jnp.repeat(jnp.exp(log_scale), C // 8, axis=1)
    return (base * scales[:, None, :]).astype(jnp.bfloat16)


def levels(stream_key, shape, pieces, least, high):
    def one(position, blocks):
        heights = jax.random.uniform(jax.random.fold_in(jax.random.fold_in(stream_key, 6), position), (blocks,), jnp.float32, least / len(pieces), high / len(pieces))
        return jnp.repeat(jnp.exp(heights), shape[position] // blocks).reshape((-1,) + (1,) * (len(shape) - position - 1))

    level = one(*pieces[0])
    for cut in pieces[1:]:
        level = level * one(*cut)
    return level


def gaussian(rng, dims, scale, most, pieces=(), kind=jnp.bfloat16):
    values = jax.random.normal(rng, dims, jnp.float32) * scale
    if len(pieces) > 0:
        values = levels(rng, dims, pieces, -0.22, 0.18) * values
    return jnp.clip(values, min=-most, max=most).astype(kind)


def setup_inputs(seed: int = 0, part: int = 0) -> dict:
    arg_keys = jax.random.split(jax.random.key(seed), 10)
    part_keys = jax.random.split(jax.random.fold_in(arg_keys[9], part), 10)
    stream = gaussian(part_keys[0], (TOKENS, D), 1.0, 6.0, ((0, 4), (1, 4)))
    norm_gain = jnp.clip(1.0 + 0.18 * jax.random.normal(arg_keys[1], (LAYERS, D), jnp.float32), 0.099609375, 1.8984375).astype(jnp.bfloat16)
    w_signal = gaussian(arg_keys[2], (LAYERS, D, C), D ** -0.5, 0.09375, ((1, 4), (2, 4)))
    w_gate = gaussian(arg_keys[3], (LAYERS, D, C), D ** -0.5, 0.09375, ((1, 4), (2, 4)))
    conv_taps = draw_conv_taps(jax.random.fold_in(arg_keys[9], 71), part)
    conv_bias = gaussian(arg_keys[5], (LAYERS, C), 0.5, 3.0, ((1, 4),))
    ln_gain = jnp.clip(1.0 + 0.18 * jax.random.normal(arg_keys[6], (LAYERS, C), jnp.float32), 0.099609375, 1.8984375).astype(jnp.bfloat16)
    ln_shift = gaussian(arg_keys[7], (LAYERS, C), 0.5, 3.0, ((1, 4),))
    w_out = gaussian(arg_keys[8], (LAYERS, C, D), (C // 4) ** -0.5, 0.375, ((1, 4), (2, 4)))
    return {"stream": stream, "norm_gain": norm_gain, "w_signal": w_signal, "w_gate": w_gate, "conv_taps": conv_taps, "conv_bias": conv_bias, "ln_gain": ln_gain, "ln_shift": ln_shift, "w_out": w_out}


EPS = 1e-05

def product(left, right):
    return jnp.dot(left, right, preferred_element_type=jnp.float32)

def layer_step(stream, gain, signal_w, gate_w, taps, bias, norm_g, norm_b, out_w):
    widened = stream.astype(jnp.float32)
    normed = (widened * lax.rsqrt(lax.optimization_barrier(jnp.mean(widened * widened, axis=-1, keepdims=True)) + EPS) * gain.astype(jnp.float32)).astype(jnp.bfloat16)
    signal = product(normed, signal_w)
    gate_pre = product(normed, gate_w)
    blended = (signal * jax.nn.sigmoid(gate_pre)).astype(jnp.bfloat16)
    fringe_rows = taps.shape[0] - 1
    padded = jnp.concatenate([jnp.zeros((fringe_rows, blended.shape[1]), jnp.bfloat16), blended], axis=0)
    length = blended.shape[0]
    filtered = jnp.zeros((length, blended.shape[1]), jnp.float32) + bias.astype(jnp.float32)
    tap_rows = taps.astype(jnp.float32)
    for tap_index in range(fringe_rows + 1):
        filtered = filtered + tap_rows[tap_index] * padded[tap_index:tap_index + length].astype(jnp.float32)
    average = lax.optimization_barrier(jnp.mean(filtered, axis=-1, keepdims=True))
    spread = lax.optimization_barrier(jnp.mean(filtered * filtered, axis=-1, keepdims=True)) - average * average
    scaled = (filtered - average) * lax.rsqrt(spread + EPS) * norm_g.astype(jnp.float32) + norm_b.astype(jnp.float32)
    activated = jax.nn.silu(scaled).astype(jnp.bfloat16)
    return (widened + product(activated, out_w)).astype(jnp.bfloat16)

def reference(stream, norm_gain, w_signal, w_gate, conv_taps, conv_bias, ln_gain, ln_shift, w_out):
    current = stream
    for layer_index in range(LAYERS):
        current = layer_step(current, norm_gain[layer_index], w_signal[layer_index], w_gate[layer_index], conv_taps[layer_index], conv_bias[layer_index], ln_gain[layer_index], ln_shift[layer_index], w_out[layer_index])
    return current
```

```python
import functools

import jax
import jax.numpy as jnp
from jax import lax
from jax.experimental import pallas as pl
from jax.experimental.pallas import tpu as pltpu
from jax.sharding import PartitionSpec as P

MESH = pl.DeviceIdType.MESH
EPS = 1e-05
F32 = jnp.float32
BF16 = jnp.bfloat16
SIG, GATE, OUT = 0, 1, 2
CHUNK = 32


def sigmoid(v):
    return 1.0 / (1.0 + jnp.exp(-v))


def kernel(
    sizes,
    stream, gain, w_signal, w_gate, taps, bias, ln_gain, ln_shift, w_out,
    result,
    sig_all, gate_all, out_all, feats, scaled_feats, inv, acc_sig, acc_gate,
    tail, halo, padded, filt, stat_cols, stat_rows, acts,
    load_sem, stream_sem, z_send, z_recv, y_send, y_recv,
    cross_send, cross_recv, core_send, core_recv,
    halo_send, halo_recv, stat_send, stat_recv,
):
    groups, sp, tp, layers, rows, kernel_taps, hp, width, channels = sizes
    g, s, t = lax.axis_index("grp"), lax.axis_index("sp"), lax.axis_index("tp")
    chips = tp // 2
    core, chip = lax.rem(t, 2), lax.div(t, 2)
    mate = t + 1 - 2 * core
    share = sp // tp
    banks = (sig_all, gate_all, out_all)
    held = (w_signal, w_gate, w_out)

    def load(l, k):
        return pltpu.make_async_copy(held[k].at[l], banks[k].at[l, s], load_sem.at[l, k])

    own_stream = pltpu.make_async_copy(stream, feats.at[0, t], stream_sem)
    own_stream.start()
    for l in range(layers):
        for k in range(3):
            load(l, k).start()

    barrier = pltpu.get_barrier_semaphore()

    def greet(where):
        pl.semaphore_signal(barrier, inc=1, device_id=where, device_id_type=MESH)

    @pl.when(s > 0)
    def _():
        greet({"sp": s - 1})

    @pl.when(s < sp - 1)
    def _():
        greet({"sp": s + 1})

    for i in range(1, groups):
        greet({"grp": lax.rem(g + i, groups)})
    for i in range(1, tp):
        greet({"tp": lax.rem(t + i, tp)})
    pl.semaphore_wait(
        barrier,
        jnp.where(s > 0, 1, 0) + jnp.where(s < sp - 1, 1, 0) + (groups - 1 + tp - 1),
    )

    def z_copy(l, k, shard, way):
        ref = banks[k].at[l, shard, g]
        return pltpu.make_async_remote_copy(
            src_ref=ref, dst_ref=ref,
            send_sem=z_send.at[l, k, way, shard], recv_sem=z_recv.at[l, k, shard],
            device_id={"sp": s + 1 if way == 0 else s - 1}, device_id_type=MESH,
        )

    def y_copy(l, k, shard):
        ref = banks[k].at[l, shard, g]
        return pltpu.make_async_remote_copy(
            src_ref=ref, dst_ref=ref,
            send_sem=y_send.at[l, k, shard], recv_sem=y_recv.at[l, k, shard],
            device_id={"grp": 1 - g}, device_id_type=MESH,
        )

    def own(l, k, done=False):
        if not done:
            load(l, k).wait()
        for way, there in ((0, s < sp - 1), (1, s > 0)):
            @pl.when(there)
            def _(way=way):
                copy = z_copy(l, k, s, way)
                copy.wait_send() if done else copy.start()

    def sides(d):
        return (
            (0, s - 1 - d, s - 1 - d >= 0, s < sp - 1),
            (1, s + 1 + d, s + 1 + d <= sp - 1, s > 0),
        )

    def relay(l, k, d, done=False):
        for way, shard, here, onward in sides(d):
            @pl.when(here)
            def _(way=way, shard=shard, onward=onward):
                if not done:
                    z_copy(l, k, shard, way).wait_recv()

                @pl.when(onward)
                def _():
                    copy = z_copy(l, k, shard, way)
                    copy.wait_send() if done else copy.start()

                copy = y_copy(l, k, shard)
                copy.wait_send() if done else copy.start()

    def other_half(l, k, d):
        for _, shard, here, _ in sides(d):
            @pl.when(here)
            def _(shard=shard):
                y_copy(l, k, shard).wait_recv()

    def cross_copy(buf, n, block, i):
        ref = buf.at[block]
        return pltpu.make_async_remote_copy(
            src_ref=ref, dst_ref=ref,
            send_sem=cross_send.at[n, i], recv_sem=cross_recv.at[n, block],
            device_id={"tp": lax.rem(chip + i, chips) * 2 + core}, device_id_type=MESH,
        )

    def core_copy(buf, n, block):
        ref = buf.at[block]
        return pltpu.make_async_remote_copy(
            src_ref=ref, dst_ref=ref,
            send_sem=core_send.at[n, block], recv_sem=core_recv.at[n, block],
            device_id={"tp": mate}, device_id_type=MESH,
        )

    def spread_start(buf, n):
        for i in range(1, chips):
            cross_copy(buf, n, t, i).start()
        core_copy(buf, n, t).start()

    def spread_relay(buf, n):
        for i in range(1, chips):
            block = lax.rem(chip + i, chips) * 2 + core
            cross_copy(buf, n, block, i).wait_recv()
            core_copy(buf, n, block).start()

    def spread_wait(buf, n):
        for j in range(chips):
            core_copy(buf, n, j * 2 + 1 - core).wait_recv()

    def spread_done(buf, n):
        for i in range(1, chips):
            cross_copy(buf, n, t, i).wait_send()
        for j in range(chips):
            core_copy(buf, n, j * 2 + core).wait_send()

    def stat_copy(l, i, block):
        return pltpu.make_async_remote_copy(
            src_ref=stat_rows.at[l, block], dst_ref=stat_rows.at[l, block],
            send_sem=stat_send.at[l, i], recv_sem=stat_recv.at[l, block],
            device_id={"tp": lax.rem(t + i, tp)}, device_id_type=MESH,
        )

    def halo_copy(l):
        return pltpu.make_async_remote_copy(
            src_ref=tail.at[l], dst_ref=halo.at[l],
            send_sem=halo_send.at[l], recv_sem=halo_recv.at[l],
            device_id={"sp": s + 1}, device_id_type=MESH,
        )

    def normalise(l):
        part = width // tp

        def body(c, carry):
            at = pl.ds(pl.multiple_of(c * CHUNK, CHUNK), CHUNK)
            total = jnp.zeros((CHUNK, 1), F32)
            for b in range(tp):
                x = feats[l, b, at, :].astype(F32)
                total = total + jnp.sum(x * x, axis=1, keepdims=True)
                scaled_feats[b, at, :] = (
                    x * gain[l : l + 1, b * part : (b + 1) * part].astype(F32)
                ).astype(BF16)
            inv[at, :] = jnp.broadcast_to(lax.rsqrt(total / width + EPS), (CHUNK, 128))
            return carry

        lax.fori_loop(0, rows // CHUNK, body, 0)

    local = channels // tp

    def project(l):
        for k, acc in ((SIG, acc_sig), (GATE, acc_gate)):
            def body(b, carry, k=k, acc=acc):
                w = banks[k][l, pl.ds(b * share, share)].reshape(width // tp, local)
                acc[...] += jnp.dot(scaled_feats[b], w, preferred_element_type=F32)
                return carry

            acc[...] = jnp.zeros_like(acc)
            lax.fori_loop(0, tp, body, 0)

        def blend(c, carry):
            at = pl.ds(pl.multiple_of(c * CHUNK, CHUNK), CHUNK)
            r = inv[at, 0:1]
            v = (acc_sig[at, :] * r) * sigmoid(acc_gate[at, :] * r)
            to = pl.ds(pl.multiple_of(hp + c * CHUNK, 8), CHUNK)
            padded[to, :] = v.astype(BF16).astype(F32)
            return carry

        lax.fori_loop(0, rows // CHUNK, blend, 0)
        tail[l] = padded[rows : rows + hp, :].astype(BF16)

        @pl.when(s < sp - 1)
        def _():
            halo_copy(l).start()

    def convolve(l):
        @pl.when(s > 0)
        def _():
            halo_copy(l).wait_recv()
            padded[0:hp, :] = halo[l].astype(F32)

        @pl.when(s == 0)
        def _():
            padded[0:hp, :] = jnp.zeros((hp, local), F32)

        tap_rows = taps[l].astype(F32)
        first = hp - (kernel_taps - 1)
        lane = lax.broadcasted_iota(jnp.int32, (CHUNK, 128), 1)
        for c in range(rows // CHUNK):
            low = c * CHUNK
            total = jnp.broadcast_to(bias[l : l + 1, :].astype(F32), (CHUNK, local))
            for j in range(kernel_taps):
                start = low + first + j
                total = total + tap_rows[j : j + 1, :] * padded[start : start + CHUNK, :]
            filt[low : low + CHUNK, :] = total
            one = jnp.sum(total, axis=1, keepdims=True)
            two = jnp.sum(total * total, axis=1, keepdims=True)
            stat_cols[low : low + CHUNK, :] = jnp.where(
                lane == 0, one, jnp.where(lane == 1, two, 0.0)
            )
        stat_rows[l, t] = jnp.transpose(stat_cols[...])[0:8, :]
        for i in range(1, tp):
            stat_copy(l, i, t).start()

    def activate(l):
        for i in range(1, tp):
            stat_copy(l, i, lax.rem(t + i, tp)).wait_recv()
        sums = jnp.sum(stat_rows[l], axis=0)
        stat_cols[...] = jnp.transpose(
            jnp.concatenate([sums, jnp.zeros((120, rows), F32)], axis=0)
        )
        gains, shifts = ln_gain[l : l + 1, :].astype(F32), ln_shift[l : l + 1, :].astype(F32)

        def body(c, carry):
            at = pl.ds(pl.multiple_of(c * CHUNK, CHUNK), CHUNK)
            average = stat_cols[at, 0:1] / channels
            spread = stat_cols[at, 1:2] / channels - average * average
            v = (filt[at, :] - average) * lax.rsqrt(spread + EPS) * gains + shifts
            acts[l, t, at, :] = (v * sigmoid(v)).astype(BF16)
            return carry

        lax.fori_loop(0, rows // CHUNK, body, 0)

    def update(l):
        columns = width // tp
        tile = min(256, columns)
        deep = 128

        def body(c, carry):
            at = pl.ds(pl.multiple_of(c * deep, deep), deep)
            for n in range(columns // tile):
                cut = slice(n * tile, (n + 1) * tile)
                total = feats[l, t, at, cut].astype(F32)
                for b in range(tp):
                    w = out_all[l, b * share : (b + 1) * share, :, :, cut].reshape(local, tile)
                    total = total + jnp.dot(acts[l, b, at, :], w, preferred_element_type=F32)
                if l + 1 < layers:
                    feats[l + 1, t, at, cut] = total.astype(BF16)
                else:
                    result[at, cut] = total.astype(BF16)
            return carry

        lax.fori_loop(0, rows // deep, body, 0)

    hops = range(sp - 1)
    own(0, SIG)
    own(0, GATE)
    own_stream.wait()
    spread_start(feats.at[0], 0)
    for l in range(layers):
        x_cut = [(d, k) for d in hops for k in (SIG, GATE)]
        middle = len(x_cut) - 3 if l == 0 else len(x_cut) - 2
        for i, (d, k) in enumerate(x_cut):
            if l and i == 0:
                continue
            if i == middle:
                spread_relay(feats.at[l], 2 * l)
            relay(l, k, d)
        own(l, OUT)
        spread_wait(feats.at[l], 2 * l)
        normalise(l)
        for d, k in x_cut:
            other_half(l, k, d)
        project(l)
        relay(l, OUT, 0)
        convolve(l)
        for d in hops[1:]:
            relay(l, OUT, d)
        if l + 1 < layers:
            own(l + 1, SIG)
            own(l + 1, GATE)
        activate(l)
        spread_start(acts.at[l], 2 * l + 1)
        if l + 1 < layers:
            relay(l + 1, SIG, 0)
        spread_relay(acts.at[l], 2 * l + 1)
        for d in hops:
            other_half(l, OUT, d)
        spread_wait(acts.at[l], 2 * l + 1)
        update(l)
        if l + 1 < layers:
            spread_start(feats.at[l + 1], 2 * l + 2)

    for l in range(layers):
        for k in (SIG, GATE, OUT):
            own(l, k, done=True)
            for d in hops:
                relay(l, k, d, done=True)
        spread_done(feats.at[l], 2 * l)
        spread_done(acts.at[l], 2 * l + 1)
        for i in range(1, tp):
            stat_copy(l, i, t).wait_send()

        @pl.when(s < sp - 1)
        def _(l=l):
            halo_copy(l).wait_send()


def shards(counts, stream, norm_gain, w_signal, w_gate, conv_taps, conv_bias, ln_gain, ln_shift, w_out):
    groups, sp, tp = counts
    layers, deep, local = w_signal.shape
    rows, part = stream.shape
    kernel_taps = conv_taps.shape[1]
    hp = -(-(kernel_taps - 1) // 16) * 16
    width, channels = part * tp, local * tp
    halves = lambda w: w.reshape(layers, groups, w.shape[1] // groups, w.shape[2])
    bank = lambda w: pltpu.VMEM((layers, sp, groups, w.shape[1] // groups, w.shape[2]), BF16)
    dma = lambda *shape: pltpu.SemaphoreType.DMA(shape)
    anywhere = pl.BlockSpec(memory_space=pl.ANY)
    inside = pl.BlockSpec(memory_space=pltpu.VMEM)
    return pl.pallas_call(
        functools.partial(
            kernel, (groups, sp, tp, layers, rows, kernel_taps, hp, width, channels)
        ),
        out_shape=jax.ShapeDtypeStruct(stream.shape, BF16),
        in_specs=[anywhere, inside, anywhere, anywhere, inside, inside, inside, inside, anywhere],
        out_specs=inside,
        scratch_shapes=[
            bank(w_signal), bank(w_gate), bank(w_out),
            pltpu.VMEM((layers, tp, rows, part), BF16),
            pltpu.VMEM((tp, rows, part), BF16),
            pltpu.VMEM((rows, 128), F32),
            pltpu.VMEM((rows, local), F32),
            pltpu.VMEM((rows, local), F32),
            pltpu.VMEM((layers, hp, local), BF16),
            pltpu.VMEM((layers, hp, local), BF16),
            pltpu.VMEM((hp + rows, local), F32),
            pltpu.VMEM((rows, local), F32),
            pltpu.VMEM((rows, 128), F32),
            pltpu.VMEM((layers, tp, 8, rows), F32),
            pltpu.VMEM((layers, tp, rows, local), BF16),
            dma(layers, 3), pltpu.SemaphoreType.DMA,
            dma(layers, 3, 2, sp), dma(layers, 3, sp), dma(layers, 3, sp), dma(layers, 3, sp),
            dma(2 * layers, tp), dma(2 * layers, tp), dma(2 * layers, tp), dma(2 * layers, tp),
            dma(layers), dma(layers), dma(layers, tp), dma(layers, tp),
        ],
        compiler_params=pltpu.CompilerParams(
            collective_id=0, has_side_effects=True, vmem_limit_bytes=60 * 1024 * 1024
        ),
    )(
        stream, norm_gain, halves(w_signal), halves(w_gate), conv_taps, conv_bias,
        ln_gain, ln_shift, halves(w_out),
    )


def solution(mesh):
    counts = tuple(mesh.shape[name] for name in ("grp", "sp", "tp"))
    return jax.shard_map(
        functools.partial(shards, counts),
        mesh=mesh,
        in_specs=(
            P(("grp", "sp"), "tp"),
            P(),
            P(None, "sp", "tp"),
            P(None, "sp", "tp"),
            P(None, None, "tp"),
            P(None, "tp"),
            P(None, "tp"),
            P(None, "tp"),
            P(None, "sp", "tp"),
        ),
        out_specs=P(("grp", "sp"), "tp"),
        check_vma=False,
    )
```

```python
import functools

import jax
import jax.numpy as jnp
from jax import lax
from jax.experimental import pallas as pl
from jax.experimental.pallas import tpu as pltpu
from jax.sharding import PartitionSpec as P

MESH = pl.DeviceIdType.MESH
EPS = 1e-05
F32 = jnp.float32
BF16 = jnp.bfloat16
SIG, GATE, OUT = 0, 1, 2
CHUNK = 32
PIECES = 2


def sigmoid(v):
    return 1.0 / (1.0 + jnp.exp(-v))


def kernel(
    sizes,
    stream, gain, w_signal, w_gate, taps, bias, ln_gain, ln_shift, w_out,
    result,
    sig_all, gate_all, out_all, feats, scaled_feats, inv, acc_sig, acc_gate,
    tail, halo, padded, filt, stat_cols, stat_rows, acts,
    load_sem, stream_sem, own_send, z_send, z_recv, y_send, y_recv,
    cross_send, cross_recv, core_send, core_recv,
    halo_send, halo_recv, stat_send, stat_recv,
):
    groups, sp, tp, layers, rows, kernel_taps, hp, width, channels = sizes
    g, s, t = lax.axis_index("grp"), lax.axis_index("sp"), lax.axis_index("tp")
    chips = tp // 2
    core, chip = lax.rem(t, 2), lax.div(t, 2)
    mate = t + 1 - 2 * core
    share = sp // tp
    banks = (sig_all, gate_all, out_all)
    held = (w_signal, w_gate, w_out)

    inner = (s > 0) & (s < sp - 1)
    pieces = [w.shape[2] for w in held]

    def load(l, k):
        return pltpu.make_async_copy(held[k].at[l], banks[k].at[l, s], load_sem.at[l, k])

    own_stream = pltpu.make_async_copy(stream, feats.at[0, t], stream_sem)
    own_stream.start()
    for l in range(layers):
        for k in range(3):
            load(l, k).start()

    barrier = pltpu.get_barrier_semaphore()

    def greet(where):
        pl.semaphore_signal(barrier, inc=1, device_id=where, device_id_type=MESH)

    @pl.when(s > 0)
    def _():
        greet({"sp": s - 1})

    @pl.when(s < sp - 1)
    def _():
        greet({"sp": s + 1})

    for i in range(1, groups):
        greet({"grp": lax.rem(g + i, groups)})
    for i in range(1, tp):
        greet({"tp": lax.rem(t + i, tp)})
    pl.semaphore_wait(
        barrier,
        jnp.where(s > 0, 1, 0) + jnp.where(s < sp - 1, 1, 0) + (groups - 1 + tp - 1),
    )

    def z_copy(l, k, q, shard, way, mine=False):
        ref = banks[k].at[l, shard, g, q]
        return pltpu.make_async_remote_copy(
            src_ref=ref, dst_ref=ref,
            send_sem=own_send.at[l, k, q] if mine and way else z_send.at[l, k, q, shard],
            recv_sem=z_recv.at[l, k, q, shard],
            device_id={"sp": s + 1 if way == 0 else s - 1}, device_id_type=MESH,
        )

    def y_copy(l, k, q, shard, half, where):
        ref = banks[k].at[l, shard, half, q]
        return pltpu.make_async_remote_copy(
            src_ref=ref, dst_ref=ref,
            send_sem=y_send.at[l, k, q, shard], recv_sem=y_recv.at[l, k, q, shard],
            device_id=where, device_id_type=MESH,
        )

    def own(l, k, done=False):
        if not done:
            load(l, k).wait()
        for way, there, end in ((0, s < sp - 1, s == 0), (1, s > 0, s == sp - 1)):
            @pl.when(there)
            def _(way=way, end=end):
                for q in range(pieces[k]):
                    copy = z_copy(l, k, q, s, way, True)
                    copy.wait_send() if done else copy.start()

                @pl.when(end)
                def _():
                    for q in range(pieces[k]):
                        where = {"sp": s + 1 if way == 0 else s - 1}
                        copy = y_copy(l, k, q, s, 1 - g, where)
                        copy.wait_send() if done else copy.start()

    def sides(d):
        left, right = s - 1 - d, s + 1 + d
        return (
            (0, left, left >= 0, s < sp - 1, (left > 0) | (d > 0)),
            (1, right, right <= sp - 1, s > 0, (right < sp - 1) | (d > 0)),
        )

    def relay(l, k, d, done=False):
        for way, shard, here, onward, across in sides(d):
            @pl.when(here)
            def _(way=way, shard=shard, onward=onward, across=across):
                for q in range(pieces[k]):
                    if not done:
                        z_copy(l, k, q, shard, way).wait_recv()

                    @pl.when(onward)
                    def _():
                        copy = z_copy(l, k, q, shard, way)
                        copy.wait_send() if done else copy.start()

                    @pl.when(across)
                    def _():
                        copy = y_copy(l, k, q, shard, g, {"grp": 1 - g})
                        copy.wait_send() if done else copy.start()

    def other_half(l, k, d):
        for _, shard, here, _, _ in sides(d):
            @pl.when(here)
            def _(shard=shard):
                for q in range(pieces[k]):
                    y_copy(l, k, q, shard, 1 - g, {"grp": 1 - g}).wait_recv()

    def cross_copy(buf, n, block, i):
        ref = buf.at[block]
        return pltpu.make_async_remote_copy(
            src_ref=ref, dst_ref=ref,
            send_sem=cross_send.at[n, i], recv_sem=cross_recv.at[n, block],
            device_id={"tp": lax.rem(chip + i, chips) * 2 + core}, device_id_type=MESH,
        )

    def core_copy(buf, n, block):
        ref = buf.at[block]
        return pltpu.make_async_remote_copy(
            src_ref=ref, dst_ref=ref,
            send_sem=core_send.at[n, block], recv_sem=core_recv.at[n, block],
            device_id={"tp": mate}, device_id_type=MESH,
        )

    def spread_start(buf, n):
        for i in range(1, chips):
            cross_copy(buf, n, t, i).start()
        core_copy(buf, n, t).start()

    def spread_relay(buf, n):
        for i in range(1, chips):
            block = lax.rem(chip + i, chips) * 2 + core
            cross_copy(buf, n, block, i).wait_recv()
            core_copy(buf, n, block).start()

    def spread_wait(buf, n):
        for j in range(chips):
            core_copy(buf, n, j * 2 + 1 - core).wait_recv()

    def spread_done(buf, n):
        for i in range(1, chips):
            cross_copy(buf, n, t, i).wait_send()
        for j in range(chips):
            core_copy(buf, n, j * 2 + core).wait_send()

    def stat_copy(l, i, block):
        return pltpu.make_async_remote_copy(
            src_ref=stat_rows.at[l, block], dst_ref=stat_rows.at[l, block],
            send_sem=stat_send.at[l, i], recv_sem=stat_recv.at[l, block],
            device_id={"tp": lax.rem(t + i, tp)}, device_id_type=MESH,
        )

    def halo_copy(l):
        return pltpu.make_async_remote_copy(
            src_ref=tail.at[l], dst_ref=halo.at[l],
            send_sem=halo_send.at[l], recv_sem=halo_recv.at[l],
            device_id={"sp": s + 1}, device_id_type=MESH,
        )

    def normalise(l):
        part = width // tp

        def body(c, carry):
            at = pl.ds(pl.multiple_of(c * CHUNK, CHUNK), CHUNK)
            total = jnp.zeros((CHUNK, 1), F32)
            for b in range(tp):
                x = feats[l, b, at, :].astype(F32)
                total = total + jnp.sum(x * x, axis=1, keepdims=True)
                scaled_feats[b, at, :] = (
                    x * gain[l : l + 1, b * part : (b + 1) * part].astype(F32)
                ).astype(BF16)
            inv[at, :] = jnp.broadcast_to(lax.rsqrt(total / width + EPS), (CHUNK, 128))
            return carry

        lax.fori_loop(0, rows // CHUNK, body, 0)

    local = channels // tp

    def project(l):
        for k, acc in ((SIG, acc_sig), (GATE, acc_gate)):
            def body(b, carry, k=k, acc=acc):
                w = banks[k][l, pl.ds(b * share, share)].reshape(width // tp, local)
                acc[...] += jnp.dot(scaled_feats[b], w, preferred_element_type=F32)
                return carry

            acc[...] = jnp.zeros_like(acc)
            lax.fori_loop(0, tp, body, 0)

        def blend(c, carry):
            at = pl.ds(pl.multiple_of(c * CHUNK, CHUNK), CHUNK)
            r = inv[at, 0:1]
            v = (acc_sig[at, :] * r) * sigmoid(acc_gate[at, :] * r)
            to = pl.ds(pl.multiple_of(hp + c * CHUNK, 8), CHUNK)
            padded[to, :] = v.astype(BF16).astype(F32)
            return carry

        lax.fori_loop(0, rows // CHUNK, blend, 0)
        tail[l] = padded[rows : rows + hp, :].astype(BF16)

        @pl.when(s < sp - 1)
        def _():
            halo_copy(l).start()

    def convolve(l):
        def settle():
            @pl.when(s > 0)
            def _():
                halo_copy(l).wait_recv()
                padded[0:hp, :] = halo[l].astype(F32)

            @pl.when(s == 0)
            def _():
                padded[0:hp, :] = jnp.zeros((hp, local), F32)

        tap_rows = taps[:, l, :].astype(F32)
        first = hp - (kernel_taps - 1)
        lane = lax.broadcasted_iota(jnp.int32, (CHUNK, 128), 1)
        for c in [*range(1, rows // CHUNK), 0]:
            if c == 0:
                settle()
            low = c * CHUNK
            total = jnp.broadcast_to(bias[l : l + 1, :].astype(F32), (CHUNK, local))
            for j in range(kernel_taps):
                start = low + first + j
                total = total + tap_rows[j : j + 1, :] * padded[start : start + CHUNK, :]
            filt[low : low + CHUNK, :] = total
            one = jnp.sum(total, axis=1, keepdims=True)
            two = jnp.sum(total * total, axis=1, keepdims=True)
            stat_cols[low : low + CHUNK, :] = jnp.where(
                lane == 0, one, jnp.where(lane == 1, two, 0.0)
            )
        stat_rows[l, t] = jnp.transpose(stat_cols[...])[0:8, :]
        for i in range(1, tp):
            stat_copy(l, i, t).start()

    def activate(l):
        for i in range(1, tp):
            stat_copy(l, i, lax.rem(t + i, tp)).wait_recv()
        sums = jnp.sum(stat_rows[l], axis=0)
        stat_cols[...] = jnp.transpose(
            jnp.concatenate([sums, jnp.zeros((120, rows), F32)], axis=0)
        )
        gains, shifts = ln_gain[l : l + 1, :].astype(F32), ln_shift[l : l + 1, :].astype(F32)

        def body(c, carry):
            at = pl.ds(pl.multiple_of(c * CHUNK, CHUNK), CHUNK)
            average = stat_cols[at, 0:1] / channels
            spread = stat_cols[at, 1:2] / channels - average * average
            v = (filt[at, :] - average) * lax.rsqrt(spread + EPS) * gains + shifts
            acts[l, t, at, :] = (v * sigmoid(v)).astype(BF16)
            return carry

        lax.fori_loop(0, rows // CHUNK, body, 0)

    def update(l):
        columns = width // tp
        tile = min(256, columns)
        deep = 128

        def body(c, carry):
            at = pl.ds(pl.multiple_of(c * deep, deep), deep)
            for n in range(columns // tile):
                cut = slice(n * tile, (n + 1) * tile)
                total = feats[l, t, at, cut].astype(F32)
                for b in range(tp):
                    w = out_all[l, b * share : (b + 1) * share, :, :, :, cut].reshape(local, tile)
                    total = total + jnp.dot(acts[l, b, at, :], w, preferred_element_type=F32)
                if l + 1 < layers:
                    feats[l + 1, t, at, cut] = total.astype(BF16)
                else:
                    result[at, cut] = total.astype(BF16)
            return carry

        lax.fori_loop(0, rows // deep, body, 0)

    hops = range(sp - 1)
    own(0, SIG)
    own(0, GATE)
    own_stream.wait()
    spread_start(feats.at[0], 0)
    for l in range(layers):
        x_cut = [(d, k) for d in hops for k in (SIG, GATE)]
        middle = len(x_cut) - 3 if l == 0 else len(x_cut) - 2
        for i, (d, k) in enumerate(x_cut):
            if l and i == 0:
                continue
            if i == middle:
                if l:
                    own(l, OUT)
                spread_relay(feats.at[l], 2 * l)
            relay(l, k, d)
        if l == 0:
            own(l, OUT)
        spread_wait(feats.at[l], 2 * l)
        normalise(l)
        for d, k in x_cut:
            other_half(l, k, d)
        project(l)

        @pl.when(inner)
        def _(l=l):
            for d in hops:
                relay(l, OUT, d)

        if l + 1 < layers:
            own(l + 1, SIG)
            own(l + 1, GATE)
        convolve(l)

        @pl.when(jnp.logical_not(inner))
        def _(l=l):
            for d in hops:
                relay(l, OUT, d)

        activate(l)
        spread_start(acts.at[l], 2 * l + 1)
        if l + 1 < layers:
            relay(l + 1, SIG, 0)
        spread_relay(acts.at[l], 2 * l + 1)
        for d in hops:
            other_half(l, OUT, d)
        spread_wait(acts.at[l], 2 * l + 1)
        update(l)
        if l + 1 < layers:
            spread_start(feats.at[l + 1], 2 * l + 2)

    for l in range(layers):
        for k in (SIG, GATE, OUT):
            own(l, k, done=True)
            for d in hops:
                relay(l, k, d, done=True)
        spread_done(feats.at[l], 2 * l)
        spread_done(acts.at[l], 2 * l + 1)
        for i in range(1, tp):
            stat_copy(l, i, t).wait_send()

        @pl.when(s < sp - 1)
        def _(l=l):
            halo_copy(l).wait_send()


def shards(counts, stream, norm_gain, w_signal, w_gate, conv_taps, conv_bias, ln_gain, ln_shift, w_out):
    groups, sp, tp = counts
    layers, deep, local = w_signal.shape
    rows, part = stream.shape
    kernel_taps = conv_taps.shape[1]
    hp = -(-(kernel_taps - 1) // 16) * 16
    width, channels = part * tp, local * tp

    def cut(w):
        half = w.shape[1] // groups
        count = PIECES if half % (16 * PIECES) == 0 else 1
        return w.reshape(layers, groups, count, half // count, w.shape[2])

    w_signal, w_gate, w_out = cut(w_signal), cut(w_gate), cut(w_out)
    bank = lambda w: pltpu.VMEM((layers, sp) + w.shape[1:], BF16)
    most = max(w.shape[2] for w in (w_signal, w_gate, w_out))
    line = (layers, 3, most, sp)
    dma = lambda *shape: pltpu.SemaphoreType.DMA(shape)
    anywhere = pl.BlockSpec(memory_space=pl.ANY)
    inside = pl.BlockSpec(memory_space=pltpu.VMEM)
    return pl.pallas_call(
        functools.partial(
            kernel, (groups, sp, tp, layers, rows, kernel_taps, hp, width, channels)
        ),
        out_shape=jax.ShapeDtypeStruct(stream.shape, BF16),
        in_specs=[anywhere, inside, anywhere, anywhere, inside, inside, inside, inside, anywhere],
        out_specs=inside,
        scratch_shapes=[
            bank(w_signal), bank(w_gate), bank(w_out),
            pltpu.VMEM((layers, tp, rows, part), BF16),
            pltpu.VMEM((tp, rows, part), BF16),
            pltpu.VMEM((rows, 128), F32),
            pltpu.VMEM((rows, local), F32),
            pltpu.VMEM((rows, local), F32),
            pltpu.VMEM((layers, hp, local), BF16),
            pltpu.VMEM((layers, hp, local), BF16),
            pltpu.VMEM((hp + rows, local), F32),
            pltpu.VMEM((rows, local), F32),
            pltpu.VMEM((rows, 128), F32),
            pltpu.VMEM((layers, tp, 8, rows), F32),
            pltpu.VMEM((layers, tp, rows, local), BF16),
            dma(layers, 3), pltpu.SemaphoreType.DMA,
            dma(layers, 3, most), dma(*line), dma(*line), dma(*line), dma(*line),
            dma(2 * layers, tp), dma(2 * layers, tp), dma(2 * layers, tp), dma(2 * layers, tp),
            dma(layers), dma(layers), dma(layers, tp), dma(layers, tp),
        ],
        compiler_params=pltpu.CompilerParams(
            collective_id=0, has_side_effects=True, vmem_limit_bytes=60 * 1024 * 1024
        ),
    )(
        stream, norm_gain, w_signal, w_gate, jnp.transpose(conv_taps, (1, 0, 2)), conv_bias,
        ln_gain, ln_shift, w_out,
    )


def solution(mesh):
    counts = tuple(mesh.shape[name] for name in ("grp", "sp", "tp"))
    return jax.shard_map(
        functools.partial(shards, counts),
        mesh=mesh,
        in_specs=(
            P(("grp", "sp"), "tp"),
            P(),
            P(None, "sp", "tp"),
            P(None, "sp", "tp"),
            P(None, None, "tp"),
            P(None, "tp"),
            P(None, "tp"),
            P(None, "tp"),
            P(None, "sp", "tp"),
        ),
        out_specs=P(("grp", "sp"), "tp"),
        check_vma=False,
    )
```

```python
import functools

import jax
import jax.numpy as jnp
from jax import lax
from jax.experimental import pallas as pl
from jax.experimental.pallas import tpu as pltpu
from jax.sharding import PartitionSpec as P

MESH = pl.DeviceIdType.MESH
EPS = 1e-05
F32 = jnp.float32
BF16 = jnp.bfloat16
SIG, GATE, OUT = 0, 1, 2
CHUNK = 32
PIECES = 2


def sigmoid(v):
    return 1.0 / (1.0 + jnp.exp(-v))


def kernel(
    sizes,
    stream, gain, w_signal, w_gate, taps, bias, ln_gain, ln_shift, w_out,
    result,
    sig_all, gate_all, out_all, feats, scaled_feats, inv, acc_sig, acc_gate,
    tail, halo, padded, filt, stat_cols, stat_rows, acts,
    guest, sent, got, guest_sems,
    load_sem, stream_sem, own_send, z_send, z_recv, y_send, y_recv,
    cross_send, cross_recv, core_send, core_recv,
    halo_send, halo_recv, stat_send, stat_recv,
):
    groups, sp, tp, layers, rows, kernel_taps, hp, width, channels = sizes
    g, s, t = lax.axis_index("grp"), lax.axis_index("sp"), lax.axis_index("tp")
    chips = tp // 2
    core, chip = lax.rem(t, 2), lax.div(t, 2)
    mate = t + 1 - 2 * core
    share = sp // tp
    banks = (sig_all, gate_all, out_all)
    held = (w_signal, w_gate, w_out)

    inner = (s > 0) & (s < sp - 1)
    end = jnp.logical_not(inner)
    host = (s == 1) | (s == sp - 2)
    inward = jnp.where(s == 0, 1, sp - 2)
    outward = jnp.where(s == 1, 0, sp - 1)
    pieces = [w.shape[2] for w in held]

    def load(l, k):
        return pltpu.make_async_copy(held[k].at[l], banks[k].at[l, s], load_sem.at[l, k])

    own_stream = pltpu.make_async_copy(stream, feats.at[0, t], stream_sem)
    own_stream.start()
    for l in range(layers):
        for k in range(3):
            load(l, k).start()

    barrier = pltpu.get_barrier_semaphore()

    def greet(where):
        pl.semaphore_signal(barrier, inc=1, device_id=where, device_id_type=MESH)

    @pl.when(s > 0)
    def _():
        greet({"sp": s - 1})

    @pl.when(s < sp - 1)
    def _():
        greet({"sp": s + 1})

    for i in range(1, groups):
        greet({"grp": lax.rem(g + i, groups)})
    for i in range(1, tp):
        greet({"tp": lax.rem(t + i, tp)})
    pl.semaphore_wait(
        barrier,
        jnp.where(s > 0, 1, 0) + jnp.where(s < sp - 1, 1, 0) + (groups - 1 + tp - 1),
    )

    def z_copy(l, k, q, shard, way, mine=False):
        ref = banks[k].at[l, shard, g, q]
        return pltpu.make_async_remote_copy(
            src_ref=ref, dst_ref=ref,
            send_sem=own_send.at[l, k, q] if mine and way else z_send.at[l, k, q, shard],
            recv_sem=z_recv.at[l, k, q, shard],
            device_id={"sp": s + 1 if way == 0 else s - 1}, device_id_type=MESH,
        )

    def y_copy(l, k, q, shard, half, where):
        ref = banks[k].at[l, shard, half, q]
        return pltpu.make_async_remote_copy(
            src_ref=ref, dst_ref=ref,
            send_sem=y_send.at[l, k, q, shard], recv_sem=y_recv.at[l, k, q, shard],
            device_id=where, device_id_type=MESH,
        )

    def hosted(l, k):
        return l == 0 and k != OUT

    def own(l, k, done=False):
        if not done:
            load(l, k).wait()
        spare = 1 if hosted(l, k) else 0
        for way, there, last in (
            (0, s < sp - 1 - spare, s == 0), (1, s > spare, s == sp - 1)
        ):
            @pl.when(there)
            def _(way=way, last=last):
                for q in range(pieces[k]):
                    copy = z_copy(l, k, q, s, way, True)
                    copy.wait_send() if done else copy.start()

                if spare:
                    return

                @pl.when(last)
                def _():
                    for q in range(pieces[k]):
                        where = {"sp": s + 1 if way == 0 else s - 1}
                        copy = y_copy(l, k, q, s, 1 - g, where)
                        copy.wait_send() if done else copy.start()

    def sides(l, k, d):
        left, right = s - 1 - d, s + 1 + d
        if hosted(l, k):
            return (
                (0, left, (left >= 0) & inner, s < sp - 2, left >= 0),
                (1, right, (right <= sp - 1) & inner, s > 1, right <= sp - 1),
            )
        return (
            (0, left, left >= 0, s < sp - 1, (left > 0) | (d > 0)),
            (1, right, right <= sp - 1, s > 0, (right < sp - 1) | (d > 0)),
        )

    def relay(l, k, d, done=False):
        for way, shard, here, onward, across in sides(l, k, d):
            @pl.when(here)
            def _(way=way, shard=shard, onward=onward, across=across):
                for q in range(pieces[k]):
                    if not done:
                        z_copy(l, k, q, shard, way).wait_recv()

                    @pl.when(onward)
                    def _():
                        copy = z_copy(l, k, q, shard, way)
                        copy.wait_send() if done else copy.start()

                    @pl.when(across)
                    def _():
                        copy = y_copy(l, k, q, shard, g, {"grp": 1 - g})
                        copy.wait_send() if done else copy.start()

    def other_half(l, k, d):
        for _, shard, here, _, _ in sides(l, k, d):
            @pl.when(here)
            def _(shard=shard):
                for q in range(pieces[k]):
                    y_copy(l, k, q, shard, 1 - g, {"grp": 1 - g}).wait_recv()

    def cross_copy(buf, n, block, i):
        ref = buf.at[block]
        return pltpu.make_async_remote_copy(
            src_ref=ref, dst_ref=ref,
            send_sem=cross_send.at[n, i], recv_sem=cross_recv.at[n, block],
            device_id={"tp": lax.rem(chip + i, chips) * 2 + core}, device_id_type=MESH,
        )

    def core_copy(buf, n, block):
        ref = buf.at[block]
        return pltpu.make_async_remote_copy(
            src_ref=ref, dst_ref=ref,
            send_sem=core_send.at[n, block], recv_sem=core_recv.at[n, block],
            device_id={"tp": mate}, device_id_type=MESH,
        )

    def spread_start(buf, n):
        for i in range(1, chips):
            cross_copy(buf, n, t, i).start()
        core_copy(buf, n, t).start()

    def spread_relay(buf, n):
        for i in range(1, chips):
            block = lax.rem(chip + i, chips) * 2 + core
            cross_copy(buf, n, block, i).wait_recv()
            core_copy(buf, n, block).start()

    def spread_wait(buf, n):
        for j in range(chips):
            core_copy(buf, n, j * 2 + 1 - core).wait_recv()

    def spread_done(buf, n):
        for i in range(1, chips):
            cross_copy(buf, n, t, i).wait_send()
        for j in range(chips):
            core_copy(buf, n, j * 2 + core).wait_send()

    def stat_copy(l, i, block):
        return pltpu.make_async_remote_copy(
            src_ref=stat_rows.at[l, block], dst_ref=stat_rows.at[l, block],
            send_sem=stat_send.at[l, i], recv_sem=stat_recv.at[l, block],
            device_id={"tp": lax.rem(t + i, tp)}, device_id_type=MESH,
        )

    def tail_goes(l):
        return inner if l == 0 else s < sp - 1

    def halo_copy(l):
        return pltpu.make_async_remote_copy(
            src_ref=tail.at[l], dst_ref=halo.at[l],
            send_sem=halo_send.at[l], recv_sem=halo_recv.at[l],
            device_id={"sp": s + 1}, device_id_type=MESH,
        )

    def guest_copy():
        return pltpu.make_async_remote_copy(
            src_ref=feats.at[0, t], dst_ref=guest.at[t],
            send_sem=guest_sems.at[0], recv_sem=guest_sems.at[1],
            device_id={"sp": inward}, device_id_type=MESH,
        )

    def back_copy():
        return pltpu.make_async_remote_copy(
            src_ref=sent, dst_ref=got,
            send_sem=guest_sems.at[2], recv_sem=guest_sems.at[3],
            device_id={"sp": outward}, device_id_type=MESH,
        )

    def normalise(l, source):
        part = width // tp

        def body(c, carry):
            at = pl.ds(pl.multiple_of(c * CHUNK, CHUNK), CHUNK)
            total = jnp.zeros((CHUNK, 1), F32)
            for b in range(tp):
                x = source[b, at, :].astype(F32)
                total = total + jnp.sum(x * x, axis=1, keepdims=True)
                scaled_feats[b, at, :] = (
                    x * gain[l : l + 1, b * part : (b + 1) * part].astype(F32)
                ).astype(BF16)
            inv[at, :] = jnp.broadcast_to(lax.rsqrt(total / width + EPS), (CHUNK, 128))
            return carry

        lax.fori_loop(0, rows // CHUNK, body, 0)

    local = channels // tp

    def project(l, visiting=False):
        for k, acc in ((SIG, acc_sig), (GATE, acc_gate)):
            def body(b, carry, k=k, acc=acc):
                w = banks[k][l, pl.ds(b * share, share)].reshape(width // tp, local)
                acc[...] += jnp.dot(scaled_feats[b], w, preferred_element_type=F32)
                return carry

            acc[...] = jnp.zeros_like(acc)
            lax.fori_loop(0, tp, body, 0)

        def blend(c, carry):
            at = pl.ds(pl.multiple_of(c * CHUNK, CHUNK), CHUNK)
            r = inv[at, 0:1]
            v = (acc_sig[at, :] * r) * sigmoid(acc_gate[at, :] * r)
            to = pl.ds(pl.multiple_of(hp + c * CHUNK, 8), CHUNK)
            if visiting:
                sent[at, :] = v.astype(BF16)
            else:
                padded[to, :] = v.astype(BF16).astype(F32)
            return carry

        lax.fori_loop(0, rows // CHUNK, blend, 0)
        if not visiting:
            tail[l] = padded[rows : rows + hp, :].astype(BF16)

            @pl.when(tail_goes(l))
            def _():
                halo_copy(l).start()

    def convolve(l):
        def settle():
            @pl.when(s > (1 if l == 0 else 0))
            def _():
                halo_copy(l).wait_recv()
                padded[0:hp, :] = halo[l].astype(F32)

            if l == 0:
                @pl.when(s == 1)
                def _():
                    padded[0:hp, :] = sent[rows - hp : rows, :].astype(F32)

            @pl.when(s == 0)
            def _():
                padded[0:hp, :] = jnp.zeros((hp, local), F32)

        tap_rows = taps[:, l, :].astype(F32)
        first = hp - (kernel_taps - 1)
        lane = lax.broadcasted_iota(jnp.int32, (CHUNK, 128), 1)
        for c in [*range(1, rows // CHUNK), 0]:
            if c == 0:
                settle()
            low = c * CHUNK
            total = jnp.broadcast_to(bias[l : l + 1, :].astype(F32), (CHUNK, local))
            for j in range(kernel_taps):
                start = low + first + j
                total = total + tap_rows[j : j + 1, :] * padded[start : start + CHUNK, :]
            filt[low : low + CHUNK, :] = total
            one = jnp.sum(total, axis=1, keepdims=True)
            two = jnp.sum(total * total, axis=1, keepdims=True)
            stat_cols[low : low + CHUNK, :] = jnp.where(
                lane == 0, one, jnp.where(lane == 1, two, 0.0)
            )
        stat_rows[l, t] = jnp.transpose(stat_cols[...])[0:8, :]
        for i in range(1, tp):
            stat_copy(l, i, t).start()

    def activate(l):
        for i in range(1, tp):
            stat_copy(l, i, lax.rem(t + i, tp)).wait_recv()
        sums = jnp.sum(stat_rows[l], axis=0)
        stat_cols[...] = jnp.transpose(
            jnp.concatenate([sums, jnp.zeros((120, rows), F32)], axis=0)
        )
        gains, shifts = ln_gain[l : l + 1, :].astype(F32), ln_shift[l : l + 1, :].astype(F32)

        def body(c, carry):
            at = pl.ds(pl.multiple_of(c * CHUNK, CHUNK), CHUNK)
            average = stat_cols[at, 0:1] / channels
            spread = stat_cols[at, 1:2] / channels - average * average
            v = (filt[at, :] - average) * lax.rsqrt(spread + EPS) * gains + shifts
            acts[l, t, at, :] = (v * sigmoid(v)).astype(BF16)
            return carry

        lax.fori_loop(0, rows // CHUNK, body, 0)

    def update(l):
        columns = width // tp
        tile = min(256, columns)
        deep = 128

        def body(c, carry):
            at = pl.ds(pl.multiple_of(c * deep, deep), deep)
            for n in range(columns // tile):
                cut = slice(n * tile, (n + 1) * tile)
                total = feats[l, t, at, cut].astype(F32)
                for b in range(tp):
                    w = out_all[l, b * share : (b + 1) * share, :, :, :, cut].reshape(local, tile)
                    total = total + jnp.dot(acts[l, b, at, :], w, preferred_element_type=F32)
                if l + 1 < layers:
                    feats[l + 1, t, at, cut] = total.astype(BF16)
                else:
                    result[at, cut] = total.astype(BF16)
            return carry

        lax.fori_loop(0, rows // deep, body, 0)

    hops = range(sp - 1)
    cuts = [(d, k) for d in hops for k in (SIG, GATE)]
    visit = 2 * layers

    def ahead(l):
        if l + 1 < layers:
            own(l + 1, SIG)
            own(l + 1, GATE)

    own_stream.wait()

    @pl.when(end)
    def _():
        guest_copy().start()

    own(0, SIG)
    own(0, GATE)

    @pl.when(inner)
    def _():
        spread_start(feats.at[0], 0)

    for i, (d, k) in enumerate(cuts):
        relay(0, k, d)
        if i == 1:
            own(0, OUT)

            @pl.when(host)
            def _():
                guest_copy().wait_recv()
                spread_start(guest, visit)

    @pl.when(inner)
    def _():
        spread_relay(feats.at[0], 0)
        spread_wait(feats.at[0], 0)

    for d, k in cuts:
        other_half(0, k, d)

    @pl.when(host)
    def _():
        spread_relay(guest, visit)
        spread_wait(guest, visit)
        normalise(0, guest)
        project(0, True)
        back_copy().start()

    for d in hops:
        relay(0, OUT, d)
    ahead(0)

    @pl.when(inner)
    def _():
        normalise(0, feats.at[0])
        project(0)

    @pl.when(end)
    def _():
        back_copy().wait_recv()
        padded[hp : hp + rows, :] = got[...].astype(F32)

    for l in range(layers):
        if l:
            for d, k in cuts[3:]:
                relay(l, k, d)
            own(l, OUT)
            spread_relay(feats.at[l], 2 * l)
            spread_wait(feats.at[l], 2 * l)
            normalise(l, feats.at[l])
            for d, k in cuts:
                other_half(l, k, d)
            project(l)

            @pl.when(inner)
            def _(l=l):
                for d in hops:
                    relay(l, OUT, d)

            ahead(l)
        convolve(l)
        if l:
            @pl.when(end)
            def _(l=l):
                for d in hops:
                    relay(l, OUT, d)

        more = l + 1 < layers
        if more:
            relay(l + 1, cuts[0][1], cuts[0][0])
        activate(l)
        spread_start(acts.at[l], 2 * l + 1)
        if more:
            relay(l + 1, cuts[1][1], cuts[1][0])
        spread_relay(acts.at[l], 2 * l + 1)
        for d in hops:
            other_half(l, OUT, d)
        spread_wait(acts.at[l], 2 * l + 1)
        update(l)
        if more:
            spread_start(feats.at[l + 1], 2 * l + 2)
            relay(l + 1, cuts[2][1], cuts[2][0])

    @pl.when(end)
    def _():
        guest_copy().wait_send()

    @pl.when(host)
    def _():
        back_copy().wait_send()
        spread_done(guest, visit)

    for l in range(layers):
        for k in (SIG, GATE, OUT):
            own(l, k, done=True)
            for d in hops:
                relay(l, k, d, done=True)
        @pl.when(inner if l == 0 else s >= 0)
        def _(l=l):
            spread_done(feats.at[l], 2 * l)

        spread_done(acts.at[l], 2 * l + 1)
        for i in range(1, tp):
            stat_copy(l, i, t).wait_send()

        @pl.when(tail_goes(l))
        def _(l=l):
            halo_copy(l).wait_send()


def shards(counts, stream, norm_gain, w_signal, w_gate, conv_taps, conv_bias, ln_gain, ln_shift, w_out):
    groups, sp, tp = counts
    layers, deep, local = w_signal.shape
    rows, part = stream.shape
    kernel_taps = conv_taps.shape[1]
    hp = -(-(kernel_taps - 1) // 16) * 16
    width, channels = part * tp, local * tp

    def cut(w):
        half = w.shape[1] // groups
        count = PIECES if half % (16 * PIECES) == 0 else 1
        return w.reshape(layers, groups, count, half // count, w.shape[2])

    w_signal, w_gate, w_out = cut(w_signal), cut(w_gate), cut(w_out)
    bank = lambda w: pltpu.VMEM((layers, sp) + w.shape[1:], BF16)
    most = max(w.shape[2] for w in (w_signal, w_gate, w_out))
    line = (layers, 3, most, sp)
    dma = lambda *shape: pltpu.SemaphoreType.DMA(shape)
    anywhere = pl.BlockSpec(memory_space=pl.ANY)
    inside = pl.BlockSpec(memory_space=pltpu.VMEM)
    return pl.pallas_call(
        functools.partial(
            kernel, (groups, sp, tp, layers, rows, kernel_taps, hp, width, channels)
        ),
        out_shape=jax.ShapeDtypeStruct(stream.shape, BF16),
        in_specs=[anywhere, inside, anywhere, anywhere, inside, inside, inside, inside, anywhere],
        out_specs=inside,
        scratch_shapes=[
            bank(w_signal), bank(w_gate), bank(w_out),
            pltpu.VMEM((layers, tp, rows, part), BF16),
            pltpu.VMEM((tp, rows, part), BF16),
            pltpu.VMEM((rows, 128), F32),
            pltpu.VMEM((rows, local), F32),
            pltpu.VMEM((rows, local), F32),
            pltpu.VMEM((layers, hp, local), BF16),
            pltpu.VMEM((layers, hp, local), BF16),
            pltpu.VMEM((hp + rows, local), F32),
            pltpu.VMEM((rows, local), F32),
            pltpu.VMEM((rows, 128), F32),
            pltpu.VMEM((layers, tp, 8, rows), F32),
            pltpu.VMEM((layers, tp, rows, local), BF16),
            pltpu.VMEM((tp, rows, part), BF16),
            pltpu.VMEM((rows, local), BF16),
            pltpu.VMEM((rows, local), BF16),
            dma(4),
            dma(layers, 3), pltpu.SemaphoreType.DMA,
            dma(layers, 3, most), dma(*line), dma(*line), dma(*line), dma(*line),
            dma(2 * layers + 1, tp), dma(2 * layers + 1, tp),
            dma(2 * layers + 1, tp), dma(2 * layers + 1, tp),
            dma(layers), dma(layers), dma(layers, tp), dma(layers, tp),
        ],
        compiler_params=pltpu.CompilerParams(
            collective_id=0, has_side_effects=True, vmem_limit_bytes=60 * 1024 * 1024
        ),
    )(
        stream, norm_gain, w_signal, w_gate, jnp.transpose(conv_taps, (1, 0, 2)), conv_bias,
        ln_gain, ln_shift, w_out,
    )


def solution(mesh):
    counts = tuple(mesh.shape[name] for name in ("grp", "sp", "tp"))
    return jax.shard_map(
        functools.partial(shards, counts),
        mesh=mesh,
        in_specs=(
            P(("grp", "sp"), "tp"),
            P(),
            P(None, "sp", "tp"),
            P(None, "sp", "tp"),
            P(None, None, "tp"),
            P(None, "tp"),
            P(None, "tp"),
            P(None, "tp"),
            P(None, "sp", "tp"),
        ),
        out_specs=P(("grp", "sp"), "tp"),
        check_vma=False,
    )
```

```python
import functools

import jax
import jax.numpy as jnp
from jax import lax
from jax.experimental import pallas as pl
from jax.experimental.pallas import tpu as pltpu
from jax.sharding import PartitionSpec as P

MESH = pl.DeviceIdType.MESH
EPS = 1e-05
F32 = jnp.float32
BF16 = jnp.bfloat16
SIG, GATE, OUT = 0, 1, 2
CHUNK = 32
PIECES = 2


def sigmoid(v):
    return 1.0 / (1.0 + jnp.exp(-v))


def kernel(
    sizes,
    stream, gain, w_signal, w_gate, taps, bias, ln_gain, ln_shift, w_out,
    result,
    sig_all, gate_all, out_all, feats, scaled_feats, inv, acc_sig, acc_gate,
    tail, halo, padded, filt, stat_cols, stat_rows, acts,
    load_sem, stream_sem, own_send, z_send, z_recv, y_send, y_recv,
    cross_send, cross_recv, core_send, core_recv,
    halo_send, halo_recv, stat_send, stat_recv,
):
    groups, sp, tp, layers, rows, kernel_taps, hp, width, channels = sizes
    g, s, t = lax.axis_index("grp"), lax.axis_index("sp"), lax.axis_index("tp")
    chips = tp // 2
    core, chip = lax.rem(t, 2), lax.div(t, 2)
    mate = t + 1 - 2 * core
    share = sp // tp
    banks = (sig_all, gate_all, out_all)
    held = (w_signal, w_gate, w_out)

    inner = (s > 0) & (s < sp - 1)
    pieces = [w.shape[2] for w in held]

    def load(l, k):
        return pltpu.make_async_copy(held[k].at[l], banks[k].at[l, s], load_sem.at[l, k])

    own_stream = pltpu.make_async_copy(stream, feats.at[0, t], stream_sem)
    own_stream.start()
    for l in range(layers):
        for k in range(3):
            load(l, k).start()

    barrier = pltpu.get_barrier_semaphore()

    def greet(where):
        pl.semaphore_signal(barrier, inc=1, device_id=where, device_id_type=MESH)

    @pl.when(s > 0)
    def _():
        greet({"sp": s - 1})

    @pl.when(s < sp - 1)
    def _():
        greet({"sp": s + 1})

    for i in range(1, groups):
        greet({"grp": lax.rem(g + i, groups)})
    for i in range(1, tp):
        greet({"tp": lax.rem(t + i, tp)})
    pl.semaphore_wait(
        barrier,
        jnp.where(s > 0, 1, 0) + jnp.where(s < sp - 1, 1, 0) + (groups - 1 + tp - 1),
    )

    def z_copy(l, k, q, shard, way, mine=False):
        ref = banks[k].at[l, shard, g, q]
        return pltpu.make_async_remote_copy(
            src_ref=ref, dst_ref=ref,
            send_sem=own_send.at[l, k, q] if mine and way else z_send.at[l, k, q, shard],
            recv_sem=z_recv.at[l, k, q, shard],
            device_id={"sp": s + 1 if way == 0 else s - 1}, device_id_type=MESH,
        )

    def y_copy(l, k, q, shard, half, where):
        ref = banks[k].at[l, shard, half, q]
        return pltpu.make_async_remote_copy(
            src_ref=ref, dst_ref=ref,
            send_sem=y_send.at[l, k, q, shard], recv_sem=y_recv.at[l, k, q, shard],
            device_id=where, device_id_type=MESH,
        )

    def own(l, k, done=False):
        if not done:
            load(l, k).wait()
        for way, there, end in ((0, s < sp - 1, s == 0), (1, s > 0, s == sp - 1)):
            @pl.when(there)
            def _(way=way, end=end):
                for q in range(pieces[k]):
                    copy = z_copy(l, k, q, s, way, True)
                    copy.wait_send() if done else copy.start()

                @pl.when(end)
                def _():
                    for q in range(pieces[k]):
                        where = {"sp": s + 1 if way == 0 else s - 1}
                        copy = y_copy(l, k, q, s, 1 - g, where)
                        copy.wait_send() if done else copy.start()

    def sides(d):
        left, right = s - 1 - d, s + 1 + d
        return (
            (0, left, left >= 0, s < sp - 1, (left > 0) | (d > 0)),
            (1, right, right <= sp - 1, s > 0, (right < sp - 1) | (d > 0)),
        )

    def relay(l, k, d, done=False):
        for way, shard, here, onward, across in sides(d):
            @pl.when(here)
            def _(way=way, shard=shard, onward=onward, across=across):
                for q in range(pieces[k]):
                    if not done:
                        z_copy(l, k, q, shard, way).wait_recv()

                    @pl.when(onward)
                    def _():
                        copy = z_copy(l, k, q, shard, way)
                        copy.wait_send() if done else copy.start()

                    @pl.when(across)
                    def _():
                        copy = y_copy(l, k, q, shard, g, {"grp": 1 - g})
                        copy.wait_send() if done else copy.start()

    def other_half(l, k, d):
        for _, shard, here, _, _ in sides(d):
            @pl.when(here)
            def _(shard=shard):
                for q in range(pieces[k]):
                    y_copy(l, k, q, shard, 1 - g, {"grp": 1 - g}).wait_recv()

    def cross_copy(buf, n, block, i):
        ref = buf.at[block]
        return pltpu.make_async_remote_copy(
            src_ref=ref, dst_ref=ref,
            send_sem=cross_send.at[n, i], recv_sem=cross_recv.at[n, block],
            device_id={"tp": lax.rem(chip + i, chips) * 2 + core}, device_id_type=MESH,
        )

    def core_copy(buf, n, block):
        ref = buf.at[block]
        return pltpu.make_async_remote_copy(
            src_ref=ref, dst_ref=ref,
            send_sem=core_send.at[n, block], recv_sem=core_recv.at[n, block],
            device_id={"tp": mate}, device_id_type=MESH,
        )

    def spread_start(buf, n):
        for i in range(1, chips):
            cross_copy(buf, n, t, i).start()
        core_copy(buf, n, t).start()

    def spread_relay(buf, n):
        for i in range(1, chips):
            block = lax.rem(chip + i, chips) * 2 + core
            cross_copy(buf, n, block, i).wait_recv()
            core_copy(buf, n, block).start()

    def spread_wait(buf, n):
        for j in range(chips):
            core_copy(buf, n, j * 2 + 1 - core).wait_recv()

    def spread_done(buf, n):
        for i in range(1, chips):
            cross_copy(buf, n, t, i).wait_send()
        for j in range(chips):
            core_copy(buf, n, j * 2 + core).wait_send()

    def stat_copy(l, i, block):
        return pltpu.make_async_remote_copy(
            src_ref=stat_rows.at[l, block], dst_ref=stat_rows.at[l, block],
            send_sem=stat_send.at[l, i], recv_sem=stat_recv.at[l, block],
            device_id={"tp": lax.rem(t + i, tp)}, device_id_type=MESH,
        )

    def halo_copy(l):
        return pltpu.make_async_remote_copy(
            src_ref=tail.at[l], dst_ref=halo.at[l],
            send_sem=halo_send.at[l], recv_sem=halo_recv.at[l],
            device_id={"sp": s + 1}, device_id_type=MESH,
        )

    def normalise(l):
        part = width // tp

        def body(c, carry):
            at = pl.ds(pl.multiple_of(c * CHUNK, CHUNK), CHUNK)
            total = jnp.zeros((CHUNK, 1), F32)
            for b in range(tp):
                x = feats[l, b, at, :].astype(F32)
                total = total + jnp.sum(x * x, axis=1, keepdims=True)
                scaled_feats[b, at, :] = (
                    x * gain[l : l + 1, b * part : (b + 1) * part].astype(F32)
                ).astype(BF16)
            inv[at, :] = jnp.broadcast_to(lax.rsqrt(total / width + EPS), (CHUNK, 128))
            return carry

        lax.fori_loop(0, rows // CHUNK, body, 0)

    local = channels // tp

    def project(l):
        for k, acc in ((SIG, acc_sig), (GATE, acc_gate)):
            def body(b, carry, k=k, acc=acc):
                w = banks[k][l, pl.ds(b * share, share)].reshape(width // tp, local)
                acc[...] += jnp.dot(scaled_feats[b], w, preferred_element_type=F32)
                return carry

            acc[...] = jnp.zeros_like(acc)
            for d in range(sp - 1):
                other_half(l, k, d)
            lax.fori_loop(0, tp, body, 0)

        def blend(c, carry):
            at = pl.ds(pl.multiple_of(c * CHUNK, CHUNK), CHUNK)
            r = inv[at, 0:1]
            v = (acc_sig[at, :] * r) * sigmoid(acc_gate[at, :] * r)
            to = pl.ds(pl.multiple_of(hp + c * CHUNK, 8), CHUNK)
            padded[to, :] = v.astype(BF16).astype(F32)
            return carry

        lax.fori_loop(0, rows // CHUNK, blend, 0)
        tail[l] = padded[rows : rows + hp, :].astype(BF16)

        @pl.when(s < sp - 1)
        def _():
            halo_copy(l).start()

    def convolve(l):
        def settle():
            @pl.when(s > 0)
            def _():
                halo_copy(l).wait_recv()
                padded[0:hp, :] = halo[l].astype(F32)

            @pl.when(s == 0)
            def _():
                padded[0:hp, :] = jnp.zeros((hp, local), F32)

        tap_rows = taps[:, l, :].astype(F32)
        first = hp - (kernel_taps - 1)
        lane = lax.broadcasted_iota(jnp.int32, (CHUNK, 128), 1)
        for c in [*range(1, rows // CHUNK), 0]:
            if c == 0:
                settle()
            low = c * CHUNK
            total = jnp.broadcast_to(bias[l : l + 1, :].astype(F32), (CHUNK, local))
            for j in range(kernel_taps):
                start = low + first + j
                total = total + tap_rows[j : j + 1, :] * padded[start : start + CHUNK, :]
            filt[low : low + CHUNK, :] = total
            one = jnp.sum(total, axis=1, keepdims=True)
            two = jnp.sum(total * total, axis=1, keepdims=True)
            stat_cols[low : low + CHUNK, :] = jnp.where(
                lane == 0, one, jnp.where(lane == 1, two, 0.0)
            )
        stat_rows[l, t] = jnp.transpose(stat_cols[...])[0:8, :]
        for i in range(1, tp):
            stat_copy(l, i, t).start()

    def activate(l):
        for i in range(1, tp):
            stat_copy(l, i, lax.rem(t + i, tp)).wait_recv()
        sums = jnp.sum(stat_rows[l], axis=0)
        stat_cols[...] = jnp.transpose(
            jnp.concatenate([sums, jnp.zeros((120, rows), F32)], axis=0)
        )
        gains, shifts = ln_gain[l : l + 1, :].astype(F32), ln_shift[l : l + 1, :].astype(F32)

        def body(c, carry):
            at = pl.ds(pl.multiple_of(c * CHUNK, CHUNK), CHUNK)
            average = stat_cols[at, 0:1] / channels
            spread = stat_cols[at, 1:2] / channels - average * average
            v = (filt[at, :] - average) * lax.rsqrt(spread + EPS) * gains + shifts
            acts[l, t, at, :] = (v * sigmoid(v)).astype(BF16)
            return carry

        lax.fori_loop(0, rows // CHUNK, body, 0)

    def update(l):
        columns = width // tp
        tile = min(256, columns)
        deep = 128

        def body(c, carry):
            at = pl.ds(pl.multiple_of(c * deep, deep), deep)
            for n in range(columns // tile):
                cut = slice(n * tile, (n + 1) * tile)
                total = feats[l, t, at, cut].astype(F32)
                for b in range(tp):
                    w = out_all[l, b * share : (b + 1) * share, :, :, :, cut].reshape(local, tile)
                    total = total + jnp.dot(acts[l, b, at, :], w, preferred_element_type=F32)
                if l + 1 < layers:
                    feats[l + 1, t, at, cut] = total.astype(BF16)
                else:
                    result[at, cut] = total.astype(BF16)
            return carry

        lax.fori_loop(0, rows // deep, body, 0)

    hops = range(sp - 1)
    own(0, SIG)
    own(0, GATE)
    own_stream.wait()
    spread_start(feats.at[0], 0)
    for l in range(layers):
        x_cut = [(d, k) for d in hops for k in (SIG, GATE)]
        middle = len(x_cut) - 3 if l == 0 else len(x_cut) - 2
        for i, (d, k) in enumerate(x_cut):
            if l and i == 0:
                continue
            if i == middle:
                if l:
                    own(l, OUT)
                spread_relay(feats.at[l], 2 * l)
            relay(l, k, d)
        if l == 0:
            own(l, OUT)
        spread_wait(feats.at[l], 2 * l)
        normalise(l)
        project(l)

        @pl.when(inner)
        def _(l=l):
            for d in hops:
                relay(l, OUT, d)

        if l + 1 < layers:
            own(l + 1, SIG)
            own(l + 1, GATE)
        convolve(l)

        @pl.when(jnp.logical_not(inner))
        def _(l=l):
            for d in hops:
                relay(l, OUT, d)

        activate(l)
        spread_start(acts.at[l], 2 * l + 1)
        if l + 1 < layers:
            relay(l + 1, SIG, 0)
        spread_relay(acts.at[l], 2 * l + 1)
        for d in hops:
            other_half(l, OUT, d)
        spread_wait(acts.at[l], 2 * l + 1)
        update(l)
        if l + 1 < layers:
            spread_start(feats.at[l + 1], 2 * l + 2)

    for l in range(layers):
        for k in (SIG, GATE, OUT):
            own(l, k, done=True)
            for d in hops:
                relay(l, k, d, done=True)
        spread_done(feats.at[l], 2 * l)
        spread_done(acts.at[l], 2 * l + 1)
        for i in range(1, tp):
            stat_copy(l, i, t).wait_send()

        @pl.when(s < sp - 1)
        def _(l=l):
            halo_copy(l).wait_send()


def shards(counts, stream, norm_gain, w_signal, w_gate, conv_taps, conv_bias, ln_gain, ln_shift, w_out):
    groups, sp, tp = counts
    layers, deep, local = w_signal.shape
    rows, part = stream.shape
    kernel_taps = conv_taps.shape[1]
    hp = -(-(kernel_taps - 1) // 16) * 16
    width, channels = part * tp, local * tp

    def cut(w):
        half = w.shape[1] // groups
        count = PIECES if half % (16 * PIECES) == 0 else 1
        return w.reshape(layers, groups, count, half // count, w.shape[2])

    w_signal, w_gate, w_out = cut(w_signal), cut(w_gate), cut(w_out)
    bank = lambda w: pltpu.VMEM((layers, sp) + w.shape[1:], BF16)
    most = max(w.shape[2] for w in (w_signal, w_gate, w_out))
    line = (layers, 3, most, sp)
    dma = lambda *shape: pltpu.SemaphoreType.DMA(shape)
    anywhere = pl.BlockSpec(memory_space=pl.ANY)
    inside = pl.BlockSpec(memory_space=pltpu.VMEM)
    return pl.pallas_call(
        functools.partial(
            kernel, (groups, sp, tp, layers, rows, kernel_taps, hp, width, channels)
        ),
        out_shape=jax.ShapeDtypeStruct(stream.shape, BF16),
        in_specs=[anywhere, inside, anywhere, anywhere, inside, inside, inside, inside, anywhere],
        out_specs=inside,
        scratch_shapes=[
            bank(w_signal), bank(w_gate), bank(w_out),
            pltpu.VMEM((layers, tp, rows, part), BF16),
            pltpu.VMEM((tp, rows, part), BF16),
            pltpu.VMEM((rows, 128), F32),
            pltpu.VMEM((rows, local), F32),
            pltpu.VMEM((rows, local), F32),
            pltpu.VMEM((layers, hp, local), BF16),
            pltpu.VMEM((layers, hp, local), BF16),
            pltpu.VMEM((hp + rows, local), F32),
            pltpu.VMEM((rows, local), F32),
            pltpu.VMEM((rows, 128), F32),
            pltpu.VMEM((layers, tp, 8, rows), F32),
            pltpu.VMEM((layers, tp, rows, local), BF16),
            dma(layers, 3), pltpu.SemaphoreType.DMA,
            dma(layers, 3, most), dma(*line), dma(*line), dma(*line), dma(*line),
            dma(2 * layers, tp), dma(2 * layers, tp), dma(2 * layers, tp), dma(2 * layers, tp),
            dma(layers), dma(layers), dma(layers, tp), dma(layers, tp),
        ],
        compiler_params=pltpu.CompilerParams(
            collective_id=0, has_side_effects=True, vmem_limit_bytes=60 * 1024 * 1024
        ),
    )(
        stream, norm_gain, w_signal, w_gate, jnp.transpose(conv_taps, (1, 0, 2)), conv_bias,
        ln_gain, ln_shift, w_out,
    )


def solution(mesh):
    counts = tuple(mesh.shape[name] for name in ("grp", "sp", "tp"))
    return jax.shard_map(
        functools.partial(shards, counts),
        mesh=mesh,
        in_specs=(
            P(("grp", "sp"), "tp"),
            P(),
            P(None, "sp", "tp"),
            P(None, "sp", "tp"),
            P(None, None, "tp"),
            P(None, "tp"),
            P(None, "tp"),
            P(None, "tp"),
            P(None, "sp", "tp"),
        ),
        out_specs=P(("grp", "sp"), "tp"),
        check_vma=False,
    )
```
